32 devices in a mesh: ep: 4 (over y, x), tp: 8 (over z, core).
Axes of the slice: x: 2, y: 2, z: 4, core: 2. Of those that a mesh axis runs over, the one named last changes fastest.
Arguments:
- tokens: bfloat16 [2048, 2048], P('ep', 'tp'), may hold values from -6 to 6
- norm_gain: float32 [2048], replicated, may hold values from 0.1 to 1.9
- norm_shift: float32 [2048], replicated, may hold values from -3 to 3
- expert_ids: int32 [2048, 6], P('ep'), may hold values from 0 to 31, all different within a row; in each aligned block of 64 rows (0 to 63, 64 to 127, ...) at most 24 rows name the same one
- affinity: float32 [2048, 6], P('ep'), may hold values from 0.05 to 1
- expert_gate: bfloat16 [32, 2048, 512], P(('ep', 'tp')), may hold values from -0.125 to 0.125
- expert_up: bfloat16 [32, 2048, 512], P(('ep', 'tp')), may hold values from -0.125 to 0.125
- expert_down: bfloat16 [32, 512, 2048], P(('ep', 'tp')), may hold values from -0.25 to 0.25
- shared_gate: bfloat16 [512, 2048], P('tp'), may hold values from -0.125 to 0.125
- shared_up: bfloat16 [512, 2048], P('tp'), may hold values from -0.125 to 0.125
- shared_down: bfloat16 [512, 2048], replicated, may hold values from -0.25 to 0.25
Outputs:
- mixed: bfloat16 [2048, 2048], P(('ep', 'tp'))
The draws below stay inside these ranges and needn't reach their ends.
Inputs may be any that keep to these rules, and one draw needn't show every extreme that they name: `expert_ids`: each row names 6 different experts; in each aligned block of 64 rows (the rows of one device of tp) no expert is named more than 24 times, and in some blocks an expert is named exactly 24 times.
All inputs are finite; a program needn't handle non-finite values.
Results may differ from the reference program's by a relative error of at most 0.0069.
Values may be sent and summed in bfloat16 or wider, within the bound.
No kernel may reach another device: no remote copies, remote signals or barrier semaphores. Data moves between devices by JAX's collectives and lax.ppermute only.
A program may use at most 64 MiB of HBM per device.

```python
import math
import jax
import jax.numpy as jnp
import numpy as np
from jax import lax

D = 2048
HID = 512
SHARED_HID = 512
TOP_K = 6
EXPERTS = 32
ROWS_BLK = 64
SLOTS = 24
TOKENS = 2048


def block_scale(stream_key, extent, cuts, least, top_value):
    level = 1.0
    for dim, parts in cuts:
        heights = jax.random.uniform(jax.random.fold_in(jax.random.fold_in(stream_key, 6), dim), (parts,), jnp.float32, least / len(cuts), top_value / len(cuts))
        level = level * jnp.repeat(jnp.exp(heights), extent[dim] // parts).reshape((-1,) + (1,) * (len(extent) - 1 - dim))
    return level


def routed_block(key, own, number, rows, number_of, top, bound, slope):
    ranking = jax.random.permutation(key, number_of)
    crowded, ordinary = portions_of(number_of, rows * top, bound, slope, True), portions_of(number_of, rows * top, bound, slope, False)
    places = jnp.arange(number_of)

    def named(lengths, rotation):
        used = int((lengths > 0).sum())
        fixed = max(1, used // 4)
        shifted = fixed + (places - fixed + rotation * (used - fixed)) % max(1, number_of - fixed)
        return jnp.zeros((number_of,), jnp.int32).at[ranking[jnp.where(places < fixed, places, shifted)]].set(jnp.asarray(lengths, jnp.int32))

    lengths = jnp.where(number % 4 == 0, named(crowded, number // 4), named(ordinary, number - number // 4 - 1))
    mixed = jax.random.permutation(jax.random.fold_in(own, 3), number_of)
    giver, sink = mixed[0:number_of // 2 * 2:2], mixed[1:number_of // 2 * 2:2]
    room = jnp.minimum(lengths[giver] - 1, bound - lengths[sink]) // 2
    room = jnp.where((giver == ranking[0]) | (sink == ranking[0]) | (lengths[sink] == 0), 0, jnp.maximum(room, 0))
    shifted = jax.random.randint(jax.random.fold_in(own, 4), (number_of // 2,), 0, 1 << 20) % (room + 1)
    lengths = lengths.at[giver].add(-shifted).at[sink].add(shifted)
    members = jnp.searchsorted(jnp.cumsum(lengths), jnp.arange(rows * top), side="right").astype(jnp.int32)
    listing = members.reshape(top, rows).T
    listing = listing[jax.random.permutation(jax.random.fold_in(own, 1), rows)]
    rotation = jax.random.randint(jax.random.fold_in(own, 2), (rows, 1), 0, top)
    return jnp.take_along_axis(listing, (jnp.arange(top)[None, :] + rotation) % top, axis=1)


def portions_of(count, total, reach, skew, full):
    portions = [(1 << 20) // math.isqrt(standing ** skew) + 1 for standing in range(1, count + 1)]
    largest = reach if full else min(reach, max(-(-total // count), total * portions[0] // sum(portions)))
    least = 1 if total - largest >= count - 1 else 0
    given, surplus = [largest] + [least] * (count - 1), total - largest - least * (count - 1)
    while surplus > 0:
        free = [i for i in range(1, count) if given[i] < largest] or [i for i in range(1, count) if given[i] < reach]
        pool, remaining = sum([portions[i] for i in free]), surplus
        for i in free:
            more = min(reach - given[i], max(1, remaining * portions[i] // pool), surplus)
            given[i] = given[i] + more
            surplus = surplus - more
    return np.array(given)


def normal_values(rng, extent, width, most, cuts=(), kind=jnp.bfloat16):
    entries = width * jax.random.normal(rng, extent, jnp.float32)
    if cuts:
        entries = entries * block_scale(rng, extent, cuts, -0.22, 0.18)
    return jnp.clip(entries, -most, most).astype(kind)


def setup_inputs(seed: int = 0) -> dict:
    key_of = jax.random.split(jax.random.key(seed), 12)
    tokens = normal_values(key_of[0], (TOKENS, D), 1.0, 6.0, ((0, 4), (1, 8)))
    norm_gain = jnp.clip(1.0 + 0.18 * jax.random.normal(key_of[1], (D,), jnp.float32), 0.1, 1.9)
    norm_shift = normal_values(key_of[2], (D,), 0.5, 3.0, (), jnp.float32)
    expert_ids_keys = jax.random.split(jax.random.fold_in(key_of[3], 1), TOKENS // ROWS_BLK)
    expert_ids_turns = jax.random.permutation(jax.random.fold_in(key_of[3], 3), TOKENS // ROWS_BLK)
    expert_ids = jax.vmap(lambda own, number: routed_block(jax.random.fold_in(key_of[3], 2), own, number, ROWS_BLK, EXPERTS, TOP_K, SLOTS, 2))(expert_ids_keys, expert_ids_turns).reshape((TOKENS, TOP_K))
    affinity = jnp.clip(0.05 + 0.95 * jax.random.uniform(key_of[4], (TOKENS, TOP_K), jnp.float32) ** block_scale(key_of[4], (TOKENS, TOP_K), ((0, 4),), -0.2, 0.2), 0.05, 1.0)
    expert_gate = normal_values(key_of[5], (EXPERTS, D, HID), D ** -0.5, 0.125, ((0, 32),))
    expert_up = normal_values(key_of[6], (EXPERTS, D, HID), D ** -0.5, 0.125, ((0, 32),))
    expert_down = normal_values(key_of[7], (EXPERTS, HID, D), HID ** -0.5, 0.25, ((0, 32),))
    shared_gate = normal_values(key_of[8], (SHARED_HID, D), D ** -0.5, 0.125, ((0, 8),))
    shared_up = normal_values(key_of[9], (SHARED_HID, D), D ** -0.5, 0.125, ((0, 8),))
    shared_down = normal_values(key_of[10], (SHARED_HID, D), SHARED_HID ** -0.5, 0.25)
    return dict(tokens=tokens, norm_gain=norm_gain, norm_shift=norm_shift, expert_ids=expert_ids, affinity=affinity, expert_gate=expert_gate, expert_up=expert_up, expert_down=expert_down, shared_gate=shared_gate, shared_up=shared_up, shared_down=shared_down)


ROUTED_SCALE = 2.5
EPSILON = 1e-05

def pair_ranks(flat_ids, expert_count):
    onehot = flat_ids[..., None] == jnp.arange(expert_count, dtype=jnp.int32)
    running = jnp.cumsum(onehot.astype(jnp.int32), axis=-2)
    return (lax.optimization_barrier(jnp.sum(jnp.where(onehot, running, 0), axis=-1)) - 1).astype(jnp.int32)

def expert_rows(tok_rows, w_gate, w_up, w_down):
    gate_act = jnp.dot(tok_rows, w_gate, preferred_element_type=jnp.float32)
    up_act = jnp.dot(tok_rows, w_up, preferred_element_type=jnp.float32)
    hidden = (jax.nn.silu(gate_act) * up_act).astype(jnp.bfloat16)
    return jnp.dot(hidden, w_down, preferred_element_type=jnp.float32).astype(jnp.bfloat16)

def rank_block(block_ids):
    return pair_ranks(block_ids, EXPERTS)

def reference(tokens, norm_gain, norm_shift, expert_ids, affinity, expert_gate, expert_up, expert_down, shared_gate, shared_up, shared_down):
    values = tokens.astype(jnp.float32)
    center = values - lax.optimization_barrier(jnp.mean(values, axis=1, keepdims=True))
    spread = lax.optimization_barrier(jnp.mean(center * center, axis=1, keepdims=True))
    normed = (center * lax.rsqrt(spread + EPSILON) * norm_gain + norm_shift).astype(jnp.bfloat16)
    weights = affinity / lax.optimization_barrier(jnp.sum(affinity, axis=1, keepdims=True)) * ROUTED_SCALE
    contract = (((1,), (1,)), ((), ()))
    shared_g = lax.dot_general(normed, shared_gate, contract, preferred_element_type=jnp.float32)
    shared_u = lax.dot_general(normed, shared_up, contract, preferred_element_type=jnp.float32)
    shared_hidden = (jax.nn.silu(shared_g) * shared_u).astype(jnp.bfloat16)
    shared_out = jnp.dot(shared_hidden, shared_down, preferred_element_type=jnp.float32)
    blocks = TOKENS // ROWS_BLK
    block_ids = expert_ids.reshape(blocks, ROWS_BLK * TOP_K).astype(jnp.int32)
    ranks = lax.map(rank_block, block_ids)
    block_index = jnp.arange(blocks, dtype=jnp.int32)[:, None]
    dest = (block_ids * blocks + block_index) * SLOTS + ranks
    token_index = block_index * ROWS_BLK + jnp.arange(ROWS_BLK * TOP_K, dtype=jnp.int32)[None, :] // TOP_K
    token_index = jnp.broadcast_to(token_index, dest.shape)
    per_expert = blocks * SLOTS
    source_row = jnp.full((EXPERTS * per_expert,), TOKENS, jnp.int32).at[dest.reshape(-1)].set(token_index.reshape(-1))
    source_row = source_row.reshape(EXPERTS, per_expert)
    slot_weight = jnp.zeros((EXPERTS * per_expert,), jnp.float32).at[dest.reshape(-1)].set(weights.reshape(-1))
    slot_weight = slot_weight.reshape(EXPERTS, per_expert)

    def one_expert(total, inputs):
        w_gate, w_up, w_down, row_index, row_weight = inputs
        tok_rows = jnp.take(normed, row_index, axis=0, mode='fill', fill_value=0)
        result = expert_rows(tok_rows, w_gate, w_up, w_down)
        total = total.at[row_index].add(result.astype(jnp.float32) * row_weight[:, None], mode='drop')
        return (total, None)
    routed, unused = lax.scan(one_expert, jnp.zeros((TOKENS, D), jnp.float32), (expert_gate, expert_up, expert_down, source_row, slot_weight))
    return (routed + shared_out).astype(jnp.bfloat16)
```

```python
import functools

import jax
import jax.numpy as jnp
from jax import lax
from jax.experimental import pallas as pl
from jax.experimental.pallas import tpu as pltpu
from jax.sharding import PartitionSpec as P

ROUTED_SCALE = 2.5
EPSILON = 1e-05


F32 = jnp.float32
BF16 = jnp.bfloat16
VM = pl.BlockSpec(memory_space=pltpu.VMEM)
SM = pl.BlockSpec(memory_space=pltpu.SMEM)


def call(body, outs, specs, scratch=()):
    return pl.pallas_call(
        body,
        out_shape=outs,
        in_specs=specs,
        out_specs=jax.tree.map(lambda _: VM, outs),
        scratch_shapes=list(scratch),
    )


def route_body(hosts, block, cap, blocks, names, ids, ids_t, aff, key, key_t, weight_t):
    count = ids.shape[0]
    row = lax.broadcasted_iota(jnp.int32, (count, count), 0)
    col = lax.broadcasted_iota(jnp.int32, (count, count), 1)
    same = row // block == col // block
    lower = jnp.where(same & (col < row), 1.0, 0.0).astype(BF16)
    upper = jnp.where(same & (row < col), 1.0, 0.0).astype(BF16)
    here = ids[...]
    across = ids_t[...]
    share = aff[...] / jnp.sum(aff[...], axis=1, keepdims=True) * ROUTED_SCALE
    marks, marks_t, picked = [], [], []
    for k in range(hosts):
        name = names[k]
        marks.append(jnp.max(jnp.where(across == name, 1.0, 0.0), axis=0, keepdims=True))
        hit = here == name
        marks_t.append(jnp.max(jnp.where(hit, 1.0, 0.0), axis=1, keepdims=True))
        picked.append(jnp.sum(jnp.where(hit, share, 0.0), axis=1, keepdims=True))
    mark = jnp.concatenate(marks, axis=0)
    mark_t = jnp.concatenate(marks_t, axis=1)
    rank = jnp.dot(mark.astype(BF16), upper, preferred_element_type=F32)
    rank_t = jnp.dot(lower, mark_t.astype(BF16), preferred_element_type=F32)
    place = lax.broadcasted_iota(jnp.int32, mark.shape, 1) // block % blocks * cap
    place_t = lax.broadcasted_iota(jnp.int32, mark_t.shape, 0) // block % blocks * cap
    key[...] = jnp.where(mark > 0, place + rank.astype(jnp.int32), -1)
    key_t[...] = jnp.where(mark_t > 0, place_t + rank_t.astype(jnp.int32), -1)
    weight_t[...] = jnp.concatenate(picked, axis=1)


def norm_body(pieces, hosts, place, *refs):
    parts = refs[:pieces]
    gain, shift, key, shared = refs[pieces : pieces + 4]
    slots = refs[pieces + 4 : pieces + 4 + hosts]
    hidden = refs[pieces + 4 + hosts]
    rows, width = parts[0].shape
    cap = slots[0].shape[1]
    scale = 1.0 / (pieces * width)
    mean = sum(jnp.sum(p[...].astype(F32), axis=1, keepdims=True) for p in parts) * scale
    spread = 0.0
    for p in parts:
        center = p[...].astype(F32) - mean
        spread = spread + jnp.sum(center * center, axis=1, keepdims=True)
    factor = lax.rsqrt(spread * scale + EPSILON)
    order = lax.broadcasted_iota(jnp.int32, (cap, rows), 0)
    pick = jnp.concatenate(
        [jnp.where(order == key[k : k + 1, :], 1.0, 0.0) for k in range(hosts)], axis=0
    ).astype(BF16)
    act = jnp.zeros((rows, shared.shape[2]), F32)
    for n, p in enumerate(parts):
        at = place[n]
        normed = ((p[...].astype(F32) - mean) * factor * gain[at] + shift[at]).astype(BF16)
        moved = jnp.dot(pick, normed, preferred_element_type=F32).astype(BF16)
        for k in range(hosts):
            slots[k][at] = moved[k * cap : (k + 1) * cap]
        act = act + jnp.dot(normed, shared[at], preferred_element_type=F32)
    half = shared.shape[2] // 2
    gate, up = act[:, :half], act[:, half:]
    hidden[...] = (gate / (1.0 + jnp.exp(-gate)) * up).astype(BF16)


def expert_body(hosts, pieces, *refs):
    sources = refs[:hosts]
    w_gate, w_up, w_down = refs[hosts : hosts + 3]
    outs = refs[hosts + 3 : 2 * hosts + 3]
    rows = refs[2 * hosts + 3]
    cap, width = sources[0].shape[1:]
    for k in range(hosts):
        for n in range(pieces):
            rows[k * cap : (k + 1) * cap, n * width : (n + 1) * width] = sources[k][n]
    gate = jnp.dot(rows[...], w_gate[0], preferred_element_type=F32)
    up = jnp.dot(rows[...], w_up[0], preferred_element_type=F32)
    hidden = (gate / (1.0 + jnp.exp(-gate)) * up).astype(BF16)
    result = jnp.dot(hidden, w_down[0], preferred_element_type=F32).astype(BF16)
    for k in range(hosts):
        outs[k][...] = result[k * cap : (k + 1) * cap]


def combine_body(hosts, block, core, *refs):
    returned = refs[:hosts]
    key_t, weight_t, hidden, down, keep, send = refs[hosts:]
    cap = returned[0].shape[0]
    count = keep.shape[0] // block
    source = jnp.concatenate([r[...] for r in returned] + [down[...]], axis=0)
    order = lax.broadcasted_iota(jnp.int32, (block, cap), 1)
    blocks = []
    for side in range(2):
        for n in range(count):
            start = pl.multiple_of((2 * n + (core[0] + side) % 2) * block, block)
            keys = key_t[pl.ds(start, block), :]
            weights = weight_t[pl.ds(start, block), :]
            spread = [
                jnp.where(order == keys[:, k : k + 1], weights[:, k : k + 1], 0.0).astype(BF16)
                for k in range(hosts)
            ]
            blocks.append(jnp.concatenate(spread + [hidden[pl.ds(start, block), :]], axis=1))
    mix = jnp.concatenate(blocks, axis=0)
    half = count * block
    keep[...] = jnp.dot(mix[:half], source, preferred_element_type=F32)
    send[...] = jnp.dot(mix[half:], source, preferred_element_type=F32).astype(BF16)


def share_body(count, block, place, keep, other, own, *outs):
    start = pl.multiple_of(place[0] * block, block)
    own[...] = keep[pl.ds(start, block), :] + other[pl.ds(start, block), :].astype(F32)
    for k in range(1, count):
        start = pl.multiple_of(place[k] * block, block)
        outs[k - 1][...] = (
            keep[pl.ds(start, block), :] + other[pl.ds(start, block), :].astype(F32)
        ).astype(BF16)


def on_device(
    tokens,
    norm_gain,
    norm_shift,
    expert_ids,
    affinity,
    expert_gate,
    expert_up,
    expert_down,
    shared_gate,
    shared_up,
    shared_down,
):
    hosts = lax.axis_size("ep")
    members = lax.axis_size("tp")
    levels = members // 2
    rank = lax.axis_index("tp")
    level, core = rank // 2, rank % 2
    group = lax.axis_index("ep")
    count, width = tokens.shape
    top = expert_ids.shape[1]
    full = width * members
    block = count // members
    cap = max(1, 2 * block * top // (hosts * members))

    if levels % 4 == 0:
        edge = levels // 4
        inner = list(range(edge, levels - edge))
        outer = [a for a in range(levels) if a not in inner]
        chunks = [outer, inner]
    else:
        chunks = [list(range(levels))]
    per = len(chunks[0])
    blocks = 2 * per
    rows = blocks * block

    def along(k):
        return [(2 * a + s, 2 * (a ^ k) + s) for a in range(levels) for s in range(2)]

    swap = [(i, i ^ 1) for i in range(members)]

    def across(k):
        return [(i, i ^ k) for i in range(hosts)]

    def arranged(array):
        parts = array.reshape((levels, 2 * block) + array.shape[1:])
        return jnp.concatenate([parts[a] for chunk in chunks for a in chunk], axis=0)

    ids = arranged(expert_ids)
    aff = arranged(affinity)
    ordered = [jnp.concatenate([tokens[2 * block * a : 2 * block * (a + 1)] for a in chunk], axis=0) for chunk in chunks]
    names = (group ^ jnp.arange(hosts, dtype=jnp.int32)) * members + rank
    key, key_t, weight_t = call(
        functools.partial(route_body, hosts, block, cap, blocks),
        [
            jax.ShapeDtypeStruct((hosts, count), jnp.int32),
            jax.ShapeDtypeStruct((count, hosts), jnp.int32),
            jax.ShapeDtypeStruct((count, hosts), F32),
        ],
        [SM, VM, VM, VM],
    )(names, ids, ids.T, aff)
    gain = norm_gain.reshape(members, 1, width)
    shift = norm_shift.reshape(members, 1, width)
    shared = jnp.concatenate([shared_gate, shared_up], axis=0).T.reshape(members, width, -1)
    units = shared_gate.shape[0]
    down = lax.dynamic_slice_in_dim(shared_down, rank * units, units, axis=0)
    place = jnp.stack(
        [2 * (level ^ k) + (core ^ s) for k in range(levels) for s in range(2)]
    ).astype(jnp.int32)
    core_at = core.astype(jnp.int32).reshape(1)

    slots_of, hidden_of = [], []
    before = None
    for q in range(len(chunks)):
        mine = ordered[q]
        if before is not None:
            mine = lax.optimization_barrier((mine, before))[0]
        level_parts = [mine] + [lax.ppermute(mine, "tp", along(k)) for k in range(1, levels)]
        before = level_parts[1:]
        parts = []
        for part in level_parts:
            parts += [part, lax.ppermute(part, "tp", swap)]
        out = call(
            functools.partial(norm_body, members, hosts),
            [jax.ShapeDtypeStruct((members, blocks * cap, width), BF16) for _ in range(hosts)]
            + [jax.ShapeDtypeStruct((rows, units), BF16)],
            [SM] + [VM] * (members + 4),
        )(place, *parts, gain, shift, key[:, q * rows : (q + 1) * rows], shared)
        slots_of.append(
            [out[0]] + [lax.ppermute(out[k], "ep", across(k)) for k in range(1, hosts)]
        )
        hidden_of.append(out[hosts])

    returned_of = []
    for q in range(len(chunks)):
        out = call(
            functools.partial(expert_body, hosts, members),
            [jax.ShapeDtypeStruct((blocks * cap, full), BF16) for _ in range(hosts)],
            [VM] * (hosts + 3),
            [pltpu.VMEM((hosts * blocks * cap, full), BF16)],
        )(*slots_of[q], expert_gate, expert_up, expert_down)
        returned_of.append(
            [out[0]] + [lax.ppermute(out[k], "ep", across(k)) for k in range(1, hosts)]
        )

    total = 0.0
    for q, chunk in enumerate(chunks):
        span = slice(q * rows, (q + 1) * rows)
        keep, send = call(
            functools.partial(combine_body, hosts, block),
            [
                jax.ShapeDtypeStruct((per * block, full), F32),
                jax.ShapeDtypeStruct((per * block, full), BF16),
            ],
            [SM] + [VM] * (hosts + 4),
        )(core_at, *returned_of[q], key_t[span], weight_t[span], hidden_of[q], down)
        other = lax.ppermute(send, "tp", swap)
        table = jnp.array([chunk.index(a) if a in chunk else 0 for a in range(levels)], jnp.int32)
        spots = table[level ^ jnp.arange(levels, dtype=jnp.int32)]
        out = call(
            functools.partial(share_body, levels, block),
            [jax.ShapeDtypeStruct((block, full), F32)]
            + [jax.ShapeDtypeStruct((block, full), BF16) for _ in range(levels - 1)],
            [SM, VM, VM],
        )(spots, keep, other)
        owner = jnp.array([float(a in chunk) for a in range(levels)], F32)[level]
        part = out[0]
        for k in range(1, levels):
            pairs = [(2 * (a ^ k) + s, 2 * a + s) for a in chunk for s in range(2)]
            part = part + lax.ppermute(out[k], "tp", pairs).astype(F32)
        total = total + jnp.where(owner > 0, part, 0.0)
    return total.astype(BF16)


def solution(mesh):
    placed = (
        P("ep", "tp"),
        P(),
        P(),
        P("ep", None),
        P("ep", None),
        P(("ep", "tp"), None, None),
        P(("ep", "tp"), None, None),
        P(("ep", "tp"), None, None),
        P("tp", None),
        P("tp", None),
        P(),
    )
    return jax.shard_map(
        on_device, mesh=mesh, in_specs=placed, out_specs=P(("ep", "tp"), None), check_vma=False
    )
```

```python
import functools

import jax
import jax.numpy as jnp
from jax import lax
from jax.experimental import pallas as pl
from jax.experimental.pallas import tpu as pltpu
from jax.sharding import PartitionSpec as P


ROUTED_SCALE = 2.5
EPSILON = 1e-05


F32 = jnp.float32
BF16 = jnp.bfloat16
VM = pl.BlockSpec(memory_space=pltpu.VMEM)
MIB = 1 << 20


def call(body, outs, operands, limit=16, scratch=(), specs=None):
    return pl.pallas_call(
        body,
        out_shape=outs,
        in_specs=specs or [VM] * len(operands),
        out_specs=jax.tree.map(lambda _: VM, outs),
        scratch_shapes=list(scratch),
        compiler_params=pltpu.CompilerParams(vmem_limit_bytes=limit * MIB),
    )(*operands)


def silu_times(gate, up):
    return (gate / (1.0 + jnp.exp(-gate)) * up).astype(BF16)


def route_body(block, cap, chunks, ids, aff, *rest):
    outs = rest[4:-4]
    for source, target in zip(rest[:4], rest[-4:]):
        target[...] = source[...]
    hosts, levels = lax.axis_size("ep"), lax.axis_size("tp") // 2
    members = 2 * levels
    group, column = lax.axis_index("ep"), lax.axis_index("tp")
    core = lax.rem(column, 2)
    count = ids.shape[1]
    row = lax.broadcasted_iota(jnp.int32, (count, count), 0)
    col = lax.broadcasted_iota(jnp.int32, (count, count), 1)
    upper = jnp.where((row // block == col // block) & (row < col), 1.0, 0.0).astype(BF16)
    here = ids[...]
    share = aff[...]
    share = share / jnp.sum(share, axis=0, keepdims=True) * ROUTED_SCALE
    marks, picked = [], []
    for s in range(2):
        for k in range(hosts):
            hit = here == (group ^ k) * members + (column ^ s)
            marks.append(jnp.max(jnp.where(hit, 1.0, 0.0), axis=0, keepdims=True))
            picked.append(jnp.sum(jnp.where(hit, share, 0.0), axis=0, keepdims=True))
    mark = jnp.concatenate(marks, axis=0)
    weight = jnp.concatenate(picked, axis=0)
    rank = jnp.dot(mark.astype(BF16), upper, preferred_element_type=F32).astype(jnp.int32)
    rank = jnp.where(mark > 0, rank, -count)
    for q, chunk in enumerate(chunks):
        key, key_own, weight_own = outs[3 * q : 3 * q + 3]
        half = len(chunk) * block

        def arranged(array, side):
            starts = [(2 * a + side) * block for a in chunk]
            return jnp.concatenate([array[:, n : n + block] for n in starts], axis=1)

        ranks = [arranged(rank, side) for side in range(2)]
        place = lax.broadcasted_iota(jnp.int32, ranks[0].shape, 1) // block * cap
        ranks = [r + place for r in ranks]
        for side in range(2):
            key[:, side * half : (side + 1) * half] = (
                ranks[side][:hosts] + side * len(chunk) * cap * jnp.where(ranks[side][:hosts] >= 0, 1, 0)
            )
        key_own[...] = jnp.where(core == 0, ranks[0], ranks[1])
        weight_own[...] = jnp.where(core == 0, arranged(weight, 0), arranged(weight, 1))


def norm_body(hosts, *refs):
    levels = lax.axis_size("tp") // 2
    column = lax.axis_index("tp")
    level, core = column // 2, lax.rem(column, 2)
    pieces = 2 * levels
    parts = refs[:pieces]
    gain, shift, key, gate_own, up_own, gate_other, up_other = refs[pieces : pieces + 7]
    slots = refs[pieces + 7 : pieces + 7 + hosts]
    hidden = refs[pieces + 7 + hosts]
    rows, width = parts[0].shape
    cap = slots[0].shape[1]
    scale = 1.0 / (pieces * width)
    mean = sum(jnp.sum(p[...].astype(F32), axis=1, keepdims=True) for p in parts) * scale
    spread = 0.0
    for p in parts:
        center = p[...].astype(F32) - mean
        spread = spread + jnp.sum(center * center, axis=1, keepdims=True)
    factor = lax.rsqrt(spread * scale + EPSILON)
    order = lax.broadcasted_iota(jnp.int32, (cap, rows), 0)
    pick = jnp.concatenate(
        [jnp.where(order == key[k : k + 1, :], 1.0, 0.0) for k in range(hosts)], axis=0
    ).astype(BF16)
    half = rows // 2
    contract = (((1,), (1,)), ((), ()))
    acts = [0.0] * 4
    for n, p in enumerate(parts):
        at = 2 * (level ^ (n // 2)) + (core ^ (n % 2))
        span = pl.ds(pl.multiple_of(at * width, width), width)
        normed = (p[...].astype(F32) - mean) * factor * gain[:, span] + shift[:, span]
        normed = normed.astype(BF16)
        moved = jnp.dot(pick, normed, preferred_element_type=F32).astype(BF16)
        for k in range(hosts):
            slots[k][at] = moved[k * cap : (k + 1) * cap]
        owned = jnp.where(core == 0, normed[:half], normed[half:])
        for i, w in enumerate((gate_own, gate_other, up_own, up_other)):
            acts[i] = acts[i] + lax.dot_general(
                owned, w[:, span], contract, preferred_element_type=F32
            )
    gate = jnp.concatenate(acts[:2], axis=1)
    up = jnp.concatenate(acts[2:], axis=1)
    hidden[...] = silu_times(gate, up)


def expert_body(hosts, *refs):
    core = lax.rem(lax.axis_index("tp"), 2)
    sources = refs[:hosts]
    w_gate, w_up, w_down = refs[hosts : hosts + 3]
    outs = refs[hosts + 3 : 3 * hosts + 3]
    rows, near_down, arrived = refs[3 * hosts + 3 :]
    fetch = pltpu.make_async_copy(w_down.at[0], near_down, arrived)
    fetch.start()
    pieces, cap, width = sources[0].shape
    for k in range(hosts):
        for n in range(pieces):
            rows[k * cap : (k + 1) * cap, n * width : (n + 1) * width] = sources[k][n]
    gate = jnp.dot(rows[...], w_gate[0], preferred_element_type=F32)
    up = jnp.dot(rows[...], w_up[0], preferred_element_type=F32)
    hidden = silu_times(gate, up)
    fetch.wait()
    result = jnp.dot(hidden, near_down[...], preferred_element_type=F32).astype(BF16)
    half = cap // 2
    for k in range(hosts):
        low = result[k * cap : k * cap + half]
        high = result[k * cap + half : (k + 1) * cap]
        outs[k][...] = jnp.where(core == 0, low, high)
        outs[hosts + k][...] = jnp.where(core == 0, high, low)


def combine_body(chunk, *refs):
    hosts, levels = lax.axis_size("ep"), lax.axis_size("tp") // 2
    column = lax.axis_index("tp")
    level = column // 2
    returned = refs[: 2 * hosts]
    key, weight, hidden, down = refs[2 * hosts : 2 * hosts + 4]
    outs = refs[2 * hosts + 4 : 2 * hosts + 4 + levels]
    whole = refs[2 * hosts + 4 + levels]
    cap = returned[0].shape[0]
    count = key.shape[1]
    block = outs[0].shape[0]
    order = lax.broadcasted_iota(jnp.int32, (cap, count), 0)
    mix = jnp.concatenate(
        [
            jnp.where(order == key[n : n + 1, :], weight[n : n + 1, :], 0.0)
            for n in range(2 * hosts)
        ],
        axis=0,
    ).astype(BF16)
    source = jnp.concatenate([r[...] for r in returned], axis=0)
    units = hidden.shape[1] // 2
    near = down[pl.ds(pl.multiple_of(column * units, units), units), :]
    far = down[pl.ds(pl.multiple_of((column ^ 1) * units, units), units), :]
    whole[...] = lax.dot_general(
        mix, source, (((0,), (0,)), ((), ())), preferred_element_type=F32
    ) + jnp.dot(hidden[...], jnp.concatenate([near, far], axis=0), preferred_element_type=F32)
    for k in range(levels):
        spot = sum(jnp.where((level ^ k) == a, n, 0) for n, a in enumerate(chunk))
        part = whole[pl.ds(pl.multiple_of(spot * block, block), block), :]
        outs[k][...] = part.astype(outs[k].dtype)


def final_body(chunks, *refs):
    levels = lax.axis_size("tp") // 2
    level = lax.axis_index("tp") // 2
    out = refs[-1]
    for q, chunk in enumerate(chunks):
        parts = refs[q * levels : (q + 1) * levels]
        inside = functools.reduce(jnp.logical_or, [level == a for a in chunk])

        @pl.when(inside)
        def _():
            out[...] = sum(p[...].astype(F32) for p in parts).astype(BF16)


def on_device(
    tokens,
    norm_gain,
    norm_shift,
    expert_ids,
    affinity,
    expert_gate,
    expert_up,
    expert_down,
    shared_gate,
    shared_up,
    shared_down,
):
    hosts = lax.axis_size("ep")
    members = lax.axis_size("tp")
    levels = members // 2
    count, width = tokens.shape
    top = expert_ids.shape[1]
    full = width * members
    block = count // members
    cap = max(1, 2 * block * top // (hosts * members))
    units = shared_gate.shape[0]

    if levels % 4 == 0:
        edge = levels // 4
        inner = list(range(edge, levels - edge))
        chunks = [[a for a in range(levels) if a not in inner], inner]
    else:
        chunks = [list(range(levels))]
    per = len(chunks[0])
    rows = 2 * per * block
    shape = jax.ShapeDtypeStruct

    def along(k):
        return [(2 * a + s, 2 * (a ^ k) + s) for a in range(levels) for s in range(2)]

    swap = [(i, i ^ 1) for i in range(members)]

    def across(k, s):
        return [
            (g * members + i, (g ^ k) * members + (i ^ s))
            for g in range(hosts)
            for i in range(members)
        ]

    ordered = []
    for chunk in chunks:
        starts = [(2 * a + side) * block for side in range(2) for a in chunk]
        ordered.append(jnp.concatenate([tokens[n : n + block] for n in starts], axis=0))
    level_parts = [
        [mine] + [lax.ppermute(mine, "tp", along(k)) for k in range(1, levels)]
        for mine in ordered
    ]
    gate_other = lax.ppermute(shared_gate, "tp", swap)
    up_other = lax.ppermute(shared_up, "tp", swap)
    route = []
    for chunk in chunks:
        route += [
            shape((hosts, rows), jnp.int32),
            shape((2 * hosts, rows // 2), jnp.int32),
            shape((2 * hosts, rows // 2), F32),
        ]
    params = [norm_gain.reshape(1, full), norm_shift.reshape(1, full), shared_gate, shared_up]
    route += [shape(p.shape, p.dtype) for p in params]
    route = call(
        functools.partial(route_body, block, cap, chunks),
        route,
        [expert_ids.T, affinity.T] + params,
    )
    gain, shift, gate_own, up_own = route[-4:]

    slots_of, hidden_of = [], []
    for q in range(len(chunks)):
        parts = []
        for n, part in enumerate(level_parts[q]):
            if n or q:
                after = hidden_of[q - 1] if q else route[0]
                part = lax.optimization_barrier((part, after))[0]
            parts += [part, lax.ppermute(part, "tp", swap)]
        out = call(
            functools.partial(norm_body, hosts),
            [shape((members, 2 * per * cap, width), BF16) for _ in range(hosts)]
            + [shape((rows // 2, 2 * units), BF16)],
            parts + [gain, shift, route[3 * q], gate_own, up_own, gate_other, up_other],
        )
        slots_of.append(
            [out[0]]
            + [lax.ppermute(out[k], ("ep", "tp"), across(k, 0)) for k in range(1, hosts)]
        )
        hidden_of.append(out[hosts])

    returned_of = []
    for q in range(len(chunks)):
        out = call(
            functools.partial(expert_body, hosts),
            [shape((per * cap, full), BF16) for _ in range(2 * hosts)],
            slots_of[q] + [expert_gate, expert_up, expert_down],
            24,
            [
                pltpu.VMEM((hosts * 2 * per * cap, full), BF16),
                pltpu.VMEM(expert_down.shape[1:], BF16),
                pltpu.SemaphoreType.DMA(()),
            ],
            [VM] * (hosts + 2) + [pl.BlockSpec(memory_space=pltpu.HBM)],
        )
        returned_of.append(
            [out[0]]
            + [
                lax.ppermute(out[s * hosts + k], ("ep", "tp"), across(k, s))
                for s in range(2)
                for k in range(hosts)
                if s or k
            ]
        )

    sums = []
    for q, chunk in enumerate(chunks):
        out = call(
            functools.partial(combine_body, chunk),
            [shape((block, full), F32)] + [shape((block, full), BF16) for _ in range(levels - 1)],
            returned_of[q] + [route[3 * q + 1], route[3 * q + 2], hidden_of[q], shared_down],
            16,
            [pltpu.VMEM((rows // 2, full), F32)],
        )
        sums.append(out[0])
        for k in range(1, levels):
            pairs = [(2 * (a ^ k) + s, 2 * a + s) for a in chunk for s in range(2)]
            sums.append(lax.ppermute(out[k], "tp", pairs))
    return call(
        functools.partial(final_body, chunks), shape((block, full), BF16), sums
    )


def solution(mesh):
    placed = (
        P("ep", "tp"),
        P(),
        P(),
        P("ep", None),
        P("ep", None),
        P(("ep", "tp"), None, None),
        P(("ep", "tp"), None, None),
        P(("ep", "tp"), None, None),
        P("tp", None),
        P("tp", None),
        P(),
    )
    return jax.shard_map(
        on_device, mesh=mesh, in_specs=placed, out_specs=P(("ep", "tp"), None), check_vma=False
    )
```

```python
import functools

import jax
import jax.numpy as jnp
from jax import lax
from jax.experimental import pallas as pl
from jax.experimental.pallas import tpu as pltpu
from jax.sharding import PartitionSpec as P


ROUTED_SCALE = 2.5
EPSILON = 1e-05


F32 = jnp.float32
BF16 = jnp.bfloat16
VM = pl.BlockSpec(memory_space=pltpu.VMEM)
HB = pl.BlockSpec(memory_space=pltpu.HBM)
MIB = 1 << 20


def call(body, outs, operands, limit=16, scratch=(), specs=None):
    specs = specs or [VM] * len(operands)
    operands = [
        pltpu.with_memory_space_constraint(o, pltpu.HBM) if s is HB else o
        for o, s in zip(operands, specs)
    ]
    return pl.pallas_call(
        body,
        out_shape=outs,
        in_specs=specs,
        out_specs=jax.tree.map(lambda _: VM, outs),
        scratch_shapes=list(scratch),
        compiler_params=pltpu.CompilerParams(vmem_limit_bytes=limit * MIB),
    )(*operands)


def silu_times(gate, up):
    return (gate / (1.0 + jnp.exp(-gate)) * up).astype(BF16)


def route_body(block, cap, chunks, merged, ids_far, aff_far, *rest):
    ids, aff, arrived = rest[-3:]
    outs = rest[4:-7]
    moves = [
        pltpu.make_async_copy(source, target, arrived.at[n])
        for n, (source, target) in enumerate(
            zip((ids_far, aff_far) + rest[:4], (ids, aff) + rest[-7:-3])
        )
    ]
    for move in moves:
        move.start()
    hosts, levels = lax.axis_size("ep"), lax.axis_size("tp") // 2
    members = 2 * levels
    group, column = lax.axis_index("ep"), lax.axis_index("tp")
    core = lax.rem(column, 2)
    count = ids.shape[1]
    row = lax.broadcasted_iota(jnp.int32, (count, count), 0)
    col = lax.broadcasted_iota(jnp.int32, (count, count), 1)
    upper = jnp.where((row // block == col // block) & (row < col), 1.0, 0.0).astype(BF16)
    for move in moves[:2]:
        move.wait()
    here = ids[...]
    share = aff[...]
    share = share / jnp.sum(share, axis=0, keepdims=True) * ROUTED_SCALE
    marks, picked = [], []
    for s in range(2):
        for k in range(hosts):
            hit = here == (group ^ k) * members + (column ^ s)
            marks.append(jnp.max(jnp.where(hit, 1.0, 0.0), axis=0, keepdims=True))
            picked.append(jnp.sum(jnp.where(hit, share, 0.0), axis=0, keepdims=True))
    mark = jnp.concatenate(marks, axis=0)
    weight = jnp.concatenate(picked, axis=0)
    rank = jnp.dot(mark.astype(BF16), upper, preferred_element_type=F32).astype(jnp.int32)
    rank = jnp.where(mark > 0, rank, -count * count)

    def arranged(array, chunk, side):
        starts = [(2 * a + side) * block for a in chunk]
        return jnp.concatenate([array[:, n : n + block] for n in starts], axis=1)

    def placed(chunk, side):
        ranks = arranged(rank, chunk, side)
        return ranks + lax.broadcasted_iota(jnp.int32, ranks.shape, 1) // block * cap

    for q, chunk in enumerate(chunks):
        for side in range(2):
            ranks = placed(chunk, side)[:hosts] + side * len(chunk) * cap
            for n in range(len(chunk)):
                start = (2 * n + side) * block
                outs[q][:, start : start + block] = ranks[:, n * block : (n + 1) * block]
    for q, parts in enumerate(merged):
        chunk = sum([chunks[n] for n in parts], [])
        key, share = outs[len(chunks) + 2 * q : len(chunks) + 2 * q + 2]
        key[...] = jnp.where(core == 0, placed(chunk, 0), placed(chunk, 1))
        share[...] = jnp.where(core == 0, arranged(weight, chunk, 0), arranged(weight, chunk, 1))
    for move in moves[2:]:
        move.wait()


def norm_body(hosts, block, *refs):
    levels = lax.axis_size("tp") // 2
    column = lax.axis_index("tp")
    level, core = column // 2, lax.rem(column, 2)
    pieces = 2 * levels
    parts = refs[:pieces]
    gain, shift, key, gate_own, up_own, gate_other, up_other = refs[pieces : pieces + 7]
    slots = refs[pieces + 7 : pieces + 7 + hosts]
    hidden = refs[pieces + 7 + hosts]
    rows, width = parts[0].shape
    cap = slots[0].shape[1]
    scale = 1.0 / (pieces * width)
    mean = sum(jnp.sum(p[...].astype(F32), axis=1, keepdims=True) for p in parts) * scale
    spread = 0.0
    for p in parts:
        center = p[...].astype(F32) - mean
        spread = spread + jnp.sum(center * center, axis=1, keepdims=True)
    factor = lax.rsqrt(spread * scale + EPSILON)
    order = lax.broadcasted_iota(jnp.int32, (cap, rows), 0)
    pick = jnp.concatenate(
        [jnp.where(order == key[k : k + 1, :], 1.0, 0.0) for k in range(hosts)], axis=0
    ).astype(BF16)
    contract = (((1,), (1,)), ((), ()))
    acts = [0.0] * 4
    for n, p in enumerate(parts):
        at = 2 * (level ^ (n // 2)) + (core ^ (n % 2))
        span = pl.ds(pl.multiple_of(at * width, width), width)
        normed = (p[...].astype(F32) - mean) * factor * gain[:, span] + shift[:, span]
        normed = normed.astype(BF16)
        moved = jnp.dot(pick, normed, preferred_element_type=F32).astype(BF16)
        for k in range(hosts):
            slots[k][at] = moved[k * cap : (k + 1) * cap]
        sides = [
            jnp.concatenate(
                [normed[m : m + block] for m in range(s * block, rows, 2 * block)], axis=0
            )
            for s in range(2)
        ]
        owned = jnp.where(core == 0, *sides)
        for i, w in enumerate((gate_own, gate_other, up_own, up_other)):
            acts[i] = acts[i] + lax.dot_general(
                owned, w[:, span], contract, preferred_element_type=F32
            )
    gate = jnp.concatenate(acts[:2], axis=1)
    up = jnp.concatenate(acts[2:], axis=1)
    hidden[...] = silu_times(gate, up)


def expert_body(hosts, *refs):
    core = lax.rem(lax.axis_index("tp"), 2)
    w_gate, w_up, w_down, keep, give, rows, near_down, arrived = refs[-8:]
    sources = refs[:-8]
    fetch = pltpu.make_async_copy(w_down.at[0], near_down, arrived)
    fetch.start()
    start = 0
    spans = []
    for source in sources:
        pieces, cap, width = source.shape
        for n in range(pieces):
            rows[start : start + cap, n * width : (n + 1) * width] = source[n]
        spans.append((start, cap // 2))
        start += cap
    gate = jnp.dot(rows[...], w_gate[0], preferred_element_type=F32)
    up = jnp.dot(rows[...], w_up[0], preferred_element_type=F32)
    hidden = silu_times(gate, up)
    fetch.wait()
    result = jnp.dot(hidden, near_down[...], preferred_element_type=F32)
    for k in range(hosts):
        mine = [spans[n] for n in range(k, len(spans), hosts)]
        low = jnp.concatenate([result[n : n + half] for n, half in mine], axis=0)
        high = jnp.concatenate([result[n + half : n + 2 * half] for n, half in mine], axis=0)
        keep[k] = jnp.where(core == 0, low, high).astype(BF16)
        give[k] = jnp.where(core == 0, high, low).astype(BF16)


def merge_body(hosts, keep, got, *outs):
    half = keep.shape[1]
    for n, out in enumerate(outs):
        k, part = n % hosts, n // hosts
        width = out.shape[1]
        out[:half] = keep[k, :, part * width : (part + 1) * width]
        out[half:] = got[k, :, part * width : (part + 1) * width]


def combine_body(chunk, part, *refs):
    hosts, levels = lax.axis_size("ep"), lax.axis_size("tp") // 2
    column = lax.axis_index("tp")
    level = column // 2
    returned = refs[:hosts]
    key, weight, down = refs[hosts : hosts + 3]
    outs = refs[-1 - levels : -1]
    hidden = refs[hosts + 3 : -1 - levels]
    whole = refs[-1]
    cap = returned[0].shape[0] // 2
    count = key.shape[1]
    block, width = outs[0].shape
    order = lax.broadcasted_iota(jnp.int32, (cap, count), 0)
    mix = []
    for k in range(hosts):
        for n in (k, hosts + k):
            mix.append(jnp.where(order == key[n : n + 1, :], weight[n : n + 1, :], 0.0))
    mix = jnp.concatenate(mix, axis=0).astype(BF16)
    source = jnp.concatenate([r[...] for r in returned], axis=0)
    acts = jnp.concatenate([h[...] for h in hidden], axis=0)
    units = acts.shape[1] // 2
    span = slice(part * width, (part + 1) * width)
    near = down[pl.ds(pl.multiple_of(column * units, units), units), span]
    far = down[pl.ds(pl.multiple_of((column ^ 1) * units, units), units), span]
    whole[...] = lax.dot_general(
        mix, source, (((0,), (0,)), ((), ())), preferred_element_type=F32
    ) + jnp.dot(acts, jnp.concatenate([near, far], axis=0), preferred_element_type=F32)
    for k in range(levels):
        spot = sum(jnp.where((level ^ k) == a, n, 0) for n, a in enumerate(chunk))
        rows = whole[pl.ds(pl.multiple_of(spot * block, block), block), :]
        outs[k][...] = rows.astype(outs[k].dtype)


def final_body(owners, *refs):
    levels = lax.axis_size("tp") // 2
    level = lax.axis_index("tp") // 2
    out = refs[-1]
    start = 0
    for chunk, splits in owners:
        inside = functools.reduce(jnp.logical_or, [level == a for a in chunk])
        mine = refs[start : start + splits * levels]
        start += splits * levels

        @pl.when(inside)
        def _():
            width = out.shape[1] // splits
            for n in range(splits):
                parts = mine[n * levels : (n + 1) * levels]
                out[:, n * width : (n + 1) * width] = sum(
                    p[...].astype(F32) for p in parts
                ).astype(BF16)


def plan(levels):
    if levels % 4:
        return [list(range(levels))], [[0]], [1]
    edge = levels // 4
    outer = list(range(edge)), list(range(levels - edge, levels))
    return [*outer, list(range(edge, levels - edge))], [[0, 1], [2]], [1, 2]


def on_device(
    tokens,
    norm_gain,
    norm_shift,
    expert_ids,
    affinity,
    expert_gate,
    expert_up,
    expert_down,
    shared_gate,
    shared_up,
    shared_down,
):
    hosts = lax.axis_size("ep")
    members = lax.axis_size("tp")
    levels = members // 2
    count, width = tokens.shape
    top = expert_ids.shape[1]
    full = width * members
    block = count // members
    cap = max(1, 2 * block * top // (hosts * members))
    units = shared_gate.shape[0]

    chunks, merged, splits = plan(levels)
    shape = jax.ShapeDtypeStruct

    def along(k):
        return [(2 * a + s, 2 * (a ^ k) + s) for a in range(levels) for s in range(2)]

    swap = [(i, i ^ 1) for i in range(members)]

    def across(k):
        return [
            (g * members + i, (g ^ k) * members + i) for g in range(hosts) for i in range(members)
        ]

    ordered = [
        tokens[2 * block * chunk[0] : 2 * block * (chunk[-1] + 1)] for chunk in chunks
    ]
    level_parts = [
        [mine] + [lax.ppermute(mine, "tp", along(k)) for k in range(1, levels)]
        for mine in ordered
    ]
    gate_other = lax.ppermute(shared_gate, "tp", swap)
    up_other = lax.ppermute(shared_up, "tp", swap)
    route = [shape((hosts, m.shape[0]), jnp.int32) for m in ordered]
    for parts in merged:
        rows = sum(len(chunks[n]) for n in parts) * block
        route += [shape((2 * hosts, rows), jnp.int32), shape((2 * hosts, rows), F32)]
    params = [norm_gain.reshape(1, full), norm_shift.reshape(1, full), shared_gate, shared_up]
    route = call(
        functools.partial(route_body, block, cap, chunks, merged),
        route + [shape(p.shape, p.dtype) for p in params],
        [expert_ids.T, affinity.T] + params,
        scratch=[
            pltpu.VMEM((top, count), jnp.int32),
            pltpu.VMEM((top, count), F32),
            pltpu.SemaphoreType.DMA((6,)),
        ],
        specs=[HB] * 6,
    )
    gain, shift, gate_own, up_own = route[-4:]

    slots_of, hidden_of = [], []
    for q, chunk in enumerate(chunks):
        parts = []
        for n, part in enumerate(level_parts[q]):
            if n or q:
                after = hidden_of[q - 1] if q else route[0]
                part = lax.optimization_barrier((part, after))[0]
            parts += [part, lax.ppermute(part, "tp", swap)]
        out = call(
            functools.partial(norm_body, hosts, block),
            [shape((members, 2 * len(chunk) * cap, width), BF16) for _ in range(hosts)]
            + [shape((len(chunk) * block, 2 * units), BF16)],
            parts + [gain, shift, route[q], gate_own, up_own, gate_other, up_other],
        )
        slots_of.append(
            [out[0]]
            + [lax.ppermute(out[k], ("ep", "tp"), across(k)) for k in range(1, hosts)]
        )
        hidden_of.append(out[hosts])

    returned_of = []
    for q, parts in enumerate(merged):
        half = sum(len(chunks[n]) for n in parts) * cap
        keep, give = call(
            functools.partial(expert_body, hosts),
            [shape((hosts, half, full), BF16)] * 2,
            sum([slots_of[n] for n in parts], []) + [expert_gate, expert_up, expert_down],
            24,
            [
                pltpu.VMEM((hosts * 2 * half, full), BF16),
                pltpu.VMEM(expert_down.shape[1:], BF16),
                pltpu.SemaphoreType.DMA(()),
            ],
            [VM] * (hosts * len(parts) + 2) + [HB],
        )
        got = lax.ppermute(give, "tp", swap)
        out = call(
            functools.partial(merge_body, hosts),
            [shape((2 * half, full // splits[q]), BF16)]
            * (hosts * splits[q]),
            [keep, got],
        )
        returned_of.append(
            [
                [out[p * hosts]]
                + [
                    lax.ppermute(out[p * hosts + k], ("ep", "tp"), across(k))
                    for k in range(1, hosts)
                ]
                for p in range(splits[q])
            ]
        )

    sums, owners = [], []
    for q, parts in enumerate(merged):
        chunk = sum([chunks[n] for n in parts], [])
        owners.append((chunk, splits[q]))
        for p in range(splits[q]):
            part_width = full // splits[q]
            out = call(
                functools.partial(combine_body, chunk, p),
                [shape((block, part_width), F32)]
                + [shape((block, part_width), BF16) for _ in range(levels - 1)],
                returned_of[q][p]
                + [route[len(chunks) + 2 * q], route[len(chunks) + 2 * q + 1], shared_down]
                + [hidden_of[n] for n in parts],
                16,
                [pltpu.VMEM((len(chunk) * block, part_width), F32)],
            )
            sums.append(out[0])
            for k in range(1, levels):
                pairs = [(2 * (a ^ k) + s, 2 * a + s) for a in chunk for s in range(2)]
                sums.append(lax.ppermute(out[k], "tp", pairs))
    return call(functools.partial(final_body, owners), shape((block, full), BF16), sums)


def solution(mesh):
    placed = (
        P("ep", "tp"),
        P(),
        P(),
        P("ep", None),
        P("ep", None),
        P(("ep", "tp"), None, None),
        P(("ep", "tp"), None, None),
        P(("ep", "tp"), None, None),
        P("tp", None),
        P("tp", None),
        P(),
    )
    return jax.shard_map(
        on_device, mesh=mesh, in_specs=placed, out_specs=P(("ep", "tp"), None), check_vma=False
    )
```

```python
import functools

import jax
import jax.numpy as jnp
from jax import lax
from jax.experimental import pallas as pl
from jax.experimental.pallas import tpu as pltpu
from jax.sharding import PartitionSpec as P


ROUTED_SCALE = 2.5
EPSILON = 1e-05


F32 = jnp.float32
BF16 = jnp.bfloat16
VM = pl.BlockSpec(memory_space=pltpu.VMEM)
HB = pl.BlockSpec(memory_space=pltpu.HBM)
MIB = 1 << 20


def call(body, outs, operands, limit=16, scratch=(), specs=None):
    specs = specs or [VM] * len(operands)
    operands = [
        pltpu.with_memory_space_constraint(o, pltpu.HBM) if s is HB else o
        for o, s in zip(operands, specs)
    ]
    return pl.pallas_call(
        body,
        out_shape=outs,
        in_specs=specs,
        out_specs=jax.tree.map(lambda _: VM, outs),
        scratch_shapes=list(scratch),
        compiler_params=pltpu.CompilerParams(vmem_limit_bytes=limit * MIB),
    )(*operands)


def silu_times(gate, up):
    return (gate / (1.0 + jnp.exp(-gate)) * up).astype(BF16)


def route_body(block, cap, chunks, merged, ids_far, aff_far, *rest):
    ids, aff, arrived = rest[-3:]
    outs = rest[4:-7]
    moves = [
        pltpu.make_async_copy(source, target, arrived.at[n])
        for n, (source, target) in enumerate(
            zip((ids_far, aff_far) + rest[:4], (ids, aff) + rest[-7:-3])
        )
    ]
    for move in moves:
        move.start()
    hosts, levels = lax.axis_size("ep"), lax.axis_size("tp") // 2
    members = 2 * levels
    group, column = lax.axis_index("ep"), lax.axis_index("tp")
    core = lax.rem(column, 2)
    count = ids.shape[1]
    row = lax.broadcasted_iota(jnp.int32, (count, count), 0)
    col = lax.broadcasted_iota(jnp.int32, (count, count), 1)
    upper = jnp.where((row // block == col // block) & (row < col), 1.0, 0.0).astype(BF16)
    for move in moves[:2]:
        move.wait()
    here = ids[...]
    share = aff[...]
    share = share / jnp.sum(share, axis=0, keepdims=True) * ROUTED_SCALE
    marks, picked = [], []
    for s in range(2):
        for k in range(hosts):
            hit = here == (group ^ k) * members + (column ^ s)
            marks.append(jnp.max(jnp.where(hit, 1.0, 0.0), axis=0, keepdims=True))
            picked.append(jnp.sum(jnp.where(hit, share, 0.0), axis=0, keepdims=True))
    mark = jnp.concatenate(marks, axis=0)
    weight = jnp.concatenate(picked, axis=0)
    rank = jnp.dot(mark.astype(BF16), upper, preferred_element_type=F32).astype(jnp.int32)
    rank = jnp.where(mark > 0, rank, -count * count)

    def arranged(array, chunk, side):
        starts = [(2 * a + side) * block for a in chunk]
        return jnp.concatenate([array[:, n : n + block] for n in starts], axis=1)

    def placed(chunk, side):
        ranks = arranged(rank, chunk, side)
        return ranks + lax.broadcasted_iota(jnp.int32, ranks.shape, 1) // block * cap

    for q, chunk in enumerate(chunks):
        for side in range(2):
            ranks = placed(chunk, side)[:hosts] + side * len(chunk) * cap
            for n in range(len(chunk)):
                start = (2 * n + side) * block
                outs[q][:, start : start + block] = ranks[:, n * block : (n + 1) * block]
    for q, parts in enumerate(merged):
        chunk = sum([chunks[n] for n in parts], [])
        key, share = outs[len(chunks) + 2 * q : len(chunks) + 2 * q + 2]
        key[...] = jnp.where(core == 0, placed(chunk, 0), placed(chunk, 1))
        share[...] = jnp.where(core == 0, arranged(weight, chunk, 0), arranged(weight, chunk, 1))
    for move in moves[2:]:
        move.wait()


def norm_body(hosts, block, *refs):
    levels = lax.axis_size("tp") // 2
    column = lax.axis_index("tp")
    level, core = column // 2, lax.rem(column, 2)
    pieces = 2 * levels
    parts = refs[:pieces]
    gain, shift, key, gate_own, up_own, gate_other, up_other = refs[pieces : pieces + 7]
    slots = refs[pieces + 7 : pieces + 7 + hosts]
    hidden = refs[pieces + 7 + hosts]
    rows, width = parts[0].shape
    cap = slots[0].shape[1]
    scale = 1.0 / (pieces * width)
    mean = sum(jnp.sum(p[...].astype(F32), axis=1, keepdims=True) for p in parts) * scale
    spread = 0.0
    for p in parts:
        center = p[...].astype(F32) - mean
        spread = spread + jnp.sum(center * center, axis=1, keepdims=True)
    factor = lax.rsqrt(spread * scale + EPSILON)
    order = lax.broadcasted_iota(jnp.int32, (cap, rows), 0)
    pick = jnp.concatenate(
        [jnp.where(order == key[k : k + 1, :], 1.0, 0.0) for k in range(hosts)], axis=0
    ).astype(BF16)
    contract = (((1,), (1,)), ((), ()))
    acts = [0.0] * 4
    for n, p in enumerate(parts):
        at = 2 * (level ^ (n // 2)) + (core ^ (n % 2))
        span = pl.ds(pl.multiple_of(at * width, width), width)
        normed = (p[...].astype(F32) - mean) * factor * gain[:, span] + shift[:, span]
        normed = normed.astype(BF16)
        moved = jnp.dot(pick, normed, preferred_element_type=F32).astype(BF16)
        for k in range(hosts):
            slots[k][at] = moved[k * cap : (k + 1) * cap]
        sides = [
            jnp.concatenate(
                [normed[m : m + block] for m in range(s * block, rows, 2 * block)], axis=0
            )
            for s in range(2)
        ]
        owned = jnp.where(core == 0, *sides)
        for i, w in enumerate((gate_own, gate_other, up_own, up_other)):
            acts[i] = acts[i] + lax.dot_general(
                owned, w[:, span], contract, preferred_element_type=F32
            )
    gate = jnp.concatenate(acts[:2], axis=1)
    up = jnp.concatenate(acts[2:], axis=1)
    hidden[...] = silu_times(gate, up)


def expert_body(hosts, *refs):
    core = lax.rem(lax.axis_index("tp"), 2)
    w_gate, w_up, w_down, keep, give, rows, near_down, arrived = refs[-8:]
    sources = refs[:-8]
    fetch = pltpu.make_async_copy(w_down.at[0], near_down, arrived)
    fetch.start()
    start = 0
    spans = []
    for source in sources:
        pieces, cap, width = source.shape
        for n in range(pieces):
            rows[start : start + cap, n * width : (n + 1) * width] = source[n]
        spans.append((start, cap // 2))
        start += cap
    gate = jnp.dot(rows[...], w_gate[0], preferred_element_type=F32)
    up = jnp.dot(rows[...], w_up[0], preferred_element_type=F32)
    hidden = silu_times(gate, up)
    fetch.wait()
    result = jnp.dot(hidden, near_down[...], preferred_element_type=F32)
    for k in range(hosts):
        mine = [spans[n] for n in range(k, len(spans), hosts)]
        low = jnp.concatenate([result[n : n + half] for n, half in mine], axis=0)
        high = jnp.concatenate([result[n + half : n + 2 * half] for n, half in mine], axis=0)
        keep[k] = jnp.where(core == 0, low, high).astype(BF16)
        give[k] = jnp.where(core == 0, high, low).astype(BF16)


def merge_body(hosts, parts, keep, got, *outs):
    half = keep.shape[1]
    for n, out in enumerate(outs):
        k, (low, high) = n % hosts, parts[n // hosts]
        out[:half] = keep[k, :, low:high]
        out[half:] = got[k, :, low:high]


def combine_body(spots, span, *refs):
    hosts = lax.axis_size("ep")
    column = lax.axis_index("tp")
    level = column // 2
    returned = refs[:hosts]
    key, weight, down = refs[hosts : hosts + 3]
    rest = refs[hosts + 3 :]
    whole = rest[-1]
    spots = spots(level)
    outs = rest[-1 - len(spots) : -1]
    hidden = rest[: -1 - len(spots)]
    cap = returned[0].shape[0] // 2
    count = key.shape[1]
    block = outs[0].shape[0]
    order = lax.broadcasted_iota(jnp.int32, (cap, count), 0)
    mix = []
    for k in range(hosts):
        for n in (k, hosts + k):
            mix.append(jnp.where(order == key[n : n + 1, :], weight[n : n + 1, :], 0.0))
    mix = jnp.concatenate(mix, axis=0).astype(BF16)
    source = jnp.concatenate([r[...] for r in returned], axis=0)
    acts = jnp.concatenate([h[...] for h in hidden], axis=0)
    units = acts.shape[1] // 2
    near = down[pl.ds(pl.multiple_of(column * units, units), units), span]
    far = down[pl.ds(pl.multiple_of((column ^ 1) * units, units), units), span]
    whole[...] = lax.dot_general(
        mix, source, (((0,), (0,)), ((), ())), preferred_element_type=F32
    ) + jnp.dot(acts, jnp.concatenate([near, far], axis=0), preferred_element_type=F32)
    for spot, out in zip(spots, outs):
        rows = whole[pl.ds(pl.multiple_of(spot * block, block), block), :]
        out[...] = rows.astype(out.dtype)


def add_body(keep, got, wide, narrow):
    total = keep[...] + got[...].astype(F32)
    wide[...] = total
    narrow[...] = total.astype(BF16)


def final_body(owners, *refs):
    level = lax.axis_index("tp") // 2
    out = refs[-1]
    start = 0
    for chunk, spans in owners:
        inside = functools.reduce(jnp.logical_or, [level == a for a in chunk])
        mine = []
        for span, parts in spans:
            mine.append((span, refs[start : start + parts]))
            start += parts

        @pl.when(inside)
        def _(mine=mine):
            for span, parts in mine:
                out[:, span] = sum(p[...].astype(F32) for p in parts).astype(BF16)


def plan(levels, full):
    if levels % 4:
        return [list(range(levels))], [[0]], [[(0, full)]]
    edge = levels // 4
    outer = list(range(edge)), list(range(levels - edge, levels))

    def spans(*eighths):
        ends = [sum(eighths[:n]) * full // 8 for n in range(len(eighths) + 1)]
        return list(zip(ends, ends[1:]))

    return (
        [*outer, list(range(edge, levels - edge))],
        [[0, 1], [2]],
        [spans(8), spans(5, 3)],
    )


def two_steps():
    return False


def on_device(
    tokens,
    norm_gain,
    norm_shift,
    expert_ids,
    affinity,
    expert_gate,
    expert_up,
    expert_down,
    shared_gate,
    shared_up,
    shared_down,
):
    hosts = lax.axis_size("ep")
    members = lax.axis_size("tp")
    levels = members // 2
    count, width = tokens.shape
    top = expert_ids.shape[1]
    full = width * members
    block = count // members
    cap = max(1, 2 * block * top // (hosts * members))
    units = shared_gate.shape[0]

    chunks, merged, splits = plan(levels, full)
    shape = jax.ShapeDtypeStruct

    def along(k):
        return [(2 * a + s, 2 * (a ^ k) + s) for a in range(levels) for s in range(2)]

    swap = [(i, i ^ 1) for i in range(members)]

    def across(k):
        return [
            (g * members + i, (g ^ k) * members + i) for g in range(hosts) for i in range(members)
        ]

    ordered = [
        tokens[2 * block * chunk[0] : 2 * block * (chunk[-1] + 1)] for chunk in chunks
    ]
    level_parts = [
        [mine] + [lax.ppermute(mine, "tp", along(k)) for k in range(1, levels)]
        for mine in ordered
    ]
    gate_other = lax.ppermute(shared_gate, "tp", swap)
    up_other = lax.ppermute(shared_up, "tp", swap)
    route = [shape((hosts, m.shape[0]), jnp.int32) for m in ordered]
    for parts in merged:
        rows = sum(len(chunks[n]) for n in parts) * block
        route += [shape((2 * hosts, rows), jnp.int32), shape((2 * hosts, rows), F32)]
    params = [norm_gain.reshape(1, full), norm_shift.reshape(1, full), shared_gate, shared_up]
    route = call(
        functools.partial(route_body, block, cap, chunks, merged),
        route + [shape(p.shape, p.dtype) for p in params],
        [expert_ids.T, affinity.T] + params,
        scratch=[
            pltpu.VMEM((top, count), jnp.int32),
            pltpu.VMEM((top, count), F32),
            pltpu.SemaphoreType.DMA((6,)),
        ],
        specs=[HB] * 6,
    )
    gain, shift, gate_own, up_own = route[-4:]

    slots_of, hidden_of = [], []
    for q, chunk in enumerate(chunks):
        parts = []
        for n, part in enumerate(level_parts[q]):
            if n or q:
                after = hidden_of[q - 1] if q else route[0]
                part = lax.optimization_barrier((part, after))[0]
            parts += [part, lax.ppermute(part, "tp", swap)]
        out = call(
            functools.partial(norm_body, hosts, block),
            [shape((members, 2 * len(chunk) * cap, width), BF16) for _ in range(hosts)]
            + [shape((len(chunk) * block, 2 * units), BF16)],
            parts + [gain, shift, route[q], gate_own, up_own, gate_other, up_other],
        )
        slots_of.append(
            [out[0]]
            + [lax.ppermute(out[k], ("ep", "tp"), across(k)) for k in range(1, hosts)]
        )
        hidden_of.append(out[hosts])

    returned_of = []
    for q, parts in enumerate(merged):
        half = sum(len(chunks[n]) for n in parts) * cap
        keep, give = call(
            functools.partial(expert_body, hosts),
            [shape((hosts, half, full), BF16)] * 2,
            sum([slots_of[n] for n in parts], []) + [expert_gate, expert_up, expert_down],
            24,
            [
                pltpu.VMEM((hosts * 2 * half, full), BF16),
                pltpu.VMEM(expert_down.shape[1:], BF16),
                pltpu.SemaphoreType.DMA(()),
            ],
            [VM] * (hosts * len(parts) + 2) + [HB],
        )
        got = lax.ppermute(give, "tp", swap)
        out = call(
            functools.partial(merge_body, hosts, splits[q]),
            [shape((2 * half, high - low), BF16) for low, high in splits[q] for _ in range(hosts)],
            [keep, got],
        )
        returned_of.append(
            [
                [out[p * hosts]]
                + [
                    lax.ppermute(out[p * hosts + k], ("ep", "tp"), across(k))
                    for k in range(1, hosts)
                ]
                for p in range(len(splits[q]))
            ]
        )

    sums, owners = [], []
    for q, parts in enumerate(merged):
        chunk = sum([chunks[n] for n in parts], [])
        spans = []

        def at(owner, chunk=chunk):
            return sum(jnp.where(owner == a, n, 0) for n, a in enumerate(chunk))

        for p, (low, high) in enumerate(splits[q]):
            span = slice(low, high)
            if two_steps():
                spots = lambda z, at=at: [at(z % 2 * 3), at(3 - z % 2 * 3)]
            else:
                spots = lambda z, at=at: [at(z ^ k) for k in range(levels)]
            others = 1 if two_steps() else levels - 1
            out = call(
                functools.partial(combine_body, spots, span),
                [shape((block, high - low), F32)] + [shape((block, high - low), BF16)] * others,
                returned_of[q][p]
                + [route[len(chunks) + 2 * q], route[len(chunks) + 2 * q + 1], shared_down]
                + [hidden_of[n] for n in parts],
                16,
                [pltpu.VMEM((len(chunk) * block, high - low), F32)],
            )
            if two_steps():
                got = lax.ppermute(out[1], "tp", along(1))
                wide, narrow = call(
                    add_body, [shape(got.shape, F32), shape(got.shape, BF16)], [out[0], got]
                )
                pairs = [(2 * (a ^ 2) + s, 2 * a + s) for a in chunk for s in range(2)]
                tail = [wide, lax.ppermute(narrow, "tp", pairs)]
            else:
                tail = [out[0]]
                for k in range(1, levels):
                    pairs = [(2 * (a ^ k) + s, 2 * a + s) for a in chunk for s in range(2)]
                    tail.append(lax.ppermute(out[k], "tp", pairs))
            spans.append((span, len(tail)))
            sums += tail
        owners.append((chunk, spans))
    return call(functools.partial(final_body, owners), shape((block, full), BF16), sums)


def solution(mesh):
    placed = (
        P("ep", "tp"),
        P(),
        P(),
        P("ep", None),
        P("ep", None),
        P(("ep", "tp"), None, None),
        P(("ep", "tp"), None, None),
        P(("ep", "tp"), None, None),
        P("tp", None),
        P("tp", None),
        P(),
    )
    return jax.shard_map(
        on_device, mesh=mesh, in_specs=placed, out_specs=P(("ep", "tp"), None), check_vma=False
    )
```
